32 devices in a mesh: rep: 2 (over x), fs: 8 (over z, y), tp: 2 (over core).
Axes of the slice: x: 2, y: 2, z: 4, core: 2. Of those that a mesh axis runs over, the one named last changes fastest.
Arguments:
- tokens: bfloat16 [4096, 2048], P(('rep', 'fs')), may hold values from -6 to 6
- mid_tokens: bfloat16 [4096, 2048], P(('rep', 'fs')), may hold values from -6 to 6
- out_grad: bfloat16 [4096, 2048], P(('rep', 'fs')), may hold values from -6 to 6
- gate_first: bfloat16 [2048, 3072], P('fs', 'tp'), may hold values from -0.125 to 0.125
- up_first: bfloat16 [2048, 3072], P('fs', 'tp'), may hold values from -0.125 to 0.125
- down_first: bfloat16 [3072, 2048], P('tp', 'fs'), may hold values from -0.109375 to 0.109375
- gate_second: bfloat16 [2048, 3072], P('fs', 'tp'), may hold values from -0.125 to 0.125
- up_second: bfloat16 [2048, 3072], P('fs', 'tp'), may hold values from -0.125 to 0.125
- down_second: bfloat16 [3072, 2048], P('tp', 'fs'), may hold values from -0.109375 to 0.109375
Outputs:
- input_grad: bfloat16 [4096, 2048], P(('rep', 'fs'))
- down_grad: float32 [3072, 2048], P('tp', 'fs')
- row_norms: float32 [3072], P('tp')
The draws below stay inside these ranges and needn't reach their ends.
All inputs are finite; a program needn't handle non-finite values.
Results may differ from the reference program's by a relative error of at most 0.025.
Values may be sent and summed in bfloat16 or wider, within the bound.
A program may use at most 128 MiB of HBM per device.

```python
import jax
import jax.numpy as jnp
from jax import lax

D = 2048
FF = 3072
TOKENS = 4096
N_TP = 2


def strengthened(array, stream_key, source, target, parts, factor):
    def block_of(position):
        return (jnp.arange(array.shape[position]) // (array.shape[position] // parts)).reshape((-1,) + (1,) * (array.ndim - 1 - position))

    first = jax.random.permutation(stream_key, parts)[block_of(target)]
    other_side = (block_of(target) + parts // 2) % parts
    return jnp.where((block_of(source) == first) | (block_of(source) == other_side), factor * array, array)


def level_of(own_key, shape, cuts, smallest, high):
    loudness = 1.0
    for dim, parts in cuts:
        draws = jax.random.uniform(jax.random.fold_in(jax.random.fold_in(own_key, 6), dim), (parts,), jnp.float32, smallest / len(cuts), high / len(cuts))
        loudness = loudness * jnp.repeat(jnp.exp(draws), shape[dim] // parts).reshape((-1,) + (1,) * (len(shape) - 1 - dim))
    return loudness


def gaussian(stream_key, shape, deviation, most, cuts=(), held_as=jnp.bfloat16):
    values = jax.random.normal(stream_key, shape, jnp.float32) * deviation
    if len(cuts) > 0:
        values = level_of(stream_key, shape, cuts, -0.22, 0.18) * values
    return jnp.clip(values, min=-most, max=most).astype(held_as)


def noise_with(rng, shape, scale, most, pieces, heavy, kind=jnp.bfloat16):
    values = scale * jax.random.normal(rng, shape, jnp.float32)
    if pieces:
        values = values * level_of(rng, shape, pieces, -0.22, 0.18)
    return jnp.clip(strengthened(values, jax.random.fold_in(rng, 3), *heavy), -most, most).astype(kind)


def setup_inputs(seed: int = 0) -> dict:
    arg_keys = jax.random.split(jax.random.key(seed), 10)
    return {
        "tokens": gaussian(arg_keys[0], (TOKENS, D), 1.0, 6.0, ((0, 16),)),
        "mid_tokens": gaussian(arg_keys[1], (TOKENS, D), 1.0, 6.0, ((0, 16),)),
        "out_grad": noise_with(arg_keys[2], (TOKENS, D), 1.0, 6.0, ((0, 16),), (0, 1, 16, 2.0)),
        "gate_first": gaussian(arg_keys[3], (D, FF), D ** -0.5, 0.125, ((0, 8), (1, 2))),
        "up_first": gaussian(arg_keys[4], (D, FF), D ** -0.5, 0.125, ((0, 8), (1, 2))),
        "down_first": gaussian(arg_keys[5], (FF, D), FF ** -0.5, 0.109375, ((0, 2), (1, 8))),
        "gate_second": gaussian(arg_keys[6], (D, FF), D ** -0.5, 0.125, ((0, 8), (1, 2))),
        "up_second": gaussian(arg_keys[7], (D, FF), D ** -0.5, 0.125, ((0, 8), (1, 2))),
        "down_second": gaussian(arg_keys[8], (FF, D), FF ** -0.5, 0.109375, ((0, 2), (1, 8))),
    }


eps = 1e-06

def split_partials(d_gate, d_up, gate_w, up_w):
    width = d_gate.shape[1] // N_TP
    total = jnp.zeros((d_gate.shape[0], gate_w.shape[0]), jnp.float32)
    dims = (((1,), (1,)), ((), ()))
    for block in range(N_TP):
        lower = block * width
        part = lax.dot_general(d_gate[:, lower:lower + width], gate_w[:, lower:lower + width], dims, preferred_element_type=jnp.float32)
        part = part + lax.dot_general(d_up[:, lower:lower + width], up_w[:, lower:lower + width], dims, preferred_element_type=jnp.float32)
        rounded = lax.optimization_barrier(part.astype(jnp.bfloat16))
        total = total + rounded.astype(jnp.float32)
    return total

def half_back(field, carried, gate_w, up_w, down_w):
    scale = lax.rsqrt(lax.optimization_barrier(jnp.mean(field * field, axis=1, keepdims=True)) + eps)
    normed = field * scale
    normed_b = normed.astype(jnp.bfloat16)
    gate = jnp.dot(normed_b, gate_w, preferred_element_type=jnp.float32)
    upper = jnp.dot(normed_b, up_w, preferred_element_type=jnp.float32)
    back = 0.5 * lax.dot_general(carried, down_w, (((1,), (1,)), ((), ())), preferred_element_type=jnp.float32)
    logistic = jax.nn.sigmoid(gate)
    activated = gate * logistic
    hidden = (activated * upper).astype(jnp.bfloat16)
    d_gate = (back * upper * logistic * (1.0 + gate * (1.0 - logistic))).astype(jnp.bfloat16)
    d_up = (back * activated).astype(jnp.bfloat16)
    d_normed = split_partials(d_gate, d_up, gate_w, up_w)
    d_field = carried.astype(jnp.float32) + scale * (d_normed - normed * lax.optimization_barrier(jnp.mean(d_normed * normed, axis=1, keepdims=True)))
    return (d_field, hidden)

def reference(tokens, mid_tokens, out_grad, gate_first, up_first, down_first, gate_second, up_second, down_second):
    d_mid, unused = half_back(mid_tokens.astype(jnp.float32), out_grad, gate_second, up_second, down_second)
    mid_grad = d_mid.astype(jnp.bfloat16)
    d_input, hidden = half_back(tokens.astype(jnp.float32), mid_grad, gate_first, up_first, down_first)
    down_grad = 0.5 * lax.dot_general(hidden, mid_grad, (((0,), (0,)), ((), ())), preferred_element_type=jnp.float32)
    row_norms = lax.optimization_barrier(jnp.sum(down_grad * down_grad, axis=1))
    return (d_input.astype(jnp.bfloat16), down_grad, row_norms)
```

```python
import jax
import jax.numpy as jnp
from jax import lax
from jax.sharding import PartitionSpec as P

eps = 1e-06


def gathered(gate_w, up_w, down_w):
    half = gate_w.shape[1] // lax.axis_size("rep")
    start = lax.axis_index("rep") * half
    own = jnp.concatenate(
        [
            lax.dynamic_slice_in_dim(gate_w, start, half, 1),
            lax.dynamic_slice_in_dim(up_w, start, half, 1),
            lax.dynamic_slice_in_dim(down_w, start, half, 0).T,
        ],
        axis=1,
    )
    return lax.all_gather(own, "fs", axis=0, tiled=True)


def half_back(field, fields, carried, carrieds, weights):
    half = weights.shape[1] // 3
    wide = fields.astype(jnp.float32)
    normed_b = (
        wide * lax.rsqrt(jnp.mean(wide * wide, axis=1, keepdims=True) + eps)
    ).astype(jnp.bfloat16)
    gates, uppers, downs = (weights[:, i * half : (i + 1) * half] for i in range(3))
    gate = jnp.dot(normed_b, gates, preferred_element_type=jnp.float32)
    upper = jnp.dot(normed_b, uppers, preferred_element_type=jnp.float32)
    back = 0.5 * jnp.dot(carrieds, downs, preferred_element_type=jnp.float32)
    logistic = jax.nn.sigmoid(gate)
    activated = gate * logistic
    hidden = (activated * upper).astype(jnp.bfloat16)
    d_gate = (back * upper * logistic * (1.0 + gate * (1.0 - logistic))).astype(jnp.bfloat16)
    d_up = (back * activated).astype(jnp.bfloat16)
    dims = (((1,), (1,)), ((), ()))
    partial_sum = lax.dot_general(d_gate, gates, dims, preferred_element_type=jnp.float32)
    partial_sum = partial_sum + lax.dot_general(
        d_up, uppers, dims, preferred_element_type=jnp.float32
    )
    partial_sum = partial_sum.astype(jnp.bfloat16)
    n = field.shape[0]
    reps = lax.axis_size("rep")
    me = lax.axis_index("rep")
    total = lax.dynamic_slice_in_dim(partial_sum, me * n, n, 0).astype(jnp.float32)
    for k in range(1, reps):
        other = lax.rem(me + k, reps)
        sent = lax.dynamic_slice_in_dim(partial_sum, other * n, n, 0)
        got = lax.ppermute(sent, "rep", [(i, (i + k) % reps) for i in range(reps)])
        total = total + got.astype(jnp.float32)
    d_normed = lax.psum(total.astype(jnp.bfloat16), "tp").astype(jnp.float32)
    own = field.astype(jnp.float32)
    scale = lax.rsqrt(jnp.mean(own * own, axis=1, keepdims=True) + eps)
    normed = own * scale
    d_field = carried.astype(jnp.float32) + scale * (
        d_normed - normed * jnp.mean(d_normed * normed, axis=1, keepdims=True)
    )
    return d_field.astype(jnp.bfloat16), hidden


def over_rep(x):
    return lax.all_gather(x, "rep", axis=0, tiled=True)


def on_device(tokens, mid_tokens, out_grad, gate_first, up_first, down_first, gate_second, up_second, down_second):
    second = gathered(gate_second, up_second, down_second)
    first = gathered(gate_first, up_first, down_first)
    mid_grad, _ = half_back(mid_tokens, over_rep(mid_tokens), out_grad, over_rep(out_grad), second)
    mid_grads = over_rep(mid_grad)
    d_input, hidden = half_back(tokens, over_rep(tokens), mid_grad, mid_grads, first)
    partial = lax.dot_general(
        mid_grads, hidden, (((0,), (0,)), ((), ())), preferred_element_type=jnp.float32
    )
    shard = lax.psum_scatter(
        (0.5 * partial).astype(jnp.bfloat16), "fs", scatter_dimension=0, tiled=True
    )
    grad = lax.all_gather(shard, "rep", axis=1, tiled=True).astype(jnp.float32)
    norms = lax.psum(jnp.sum(grad * grad, axis=0), "fs")
    return (d_input, grad.T, norms)


def solution(mesh):
    placed = (
        P(("rep", "fs"), None),
        P(("rep", "fs"), None),
        P(("rep", "fs"), None),
        P("fs", "tp"),
        P("fs", "tp"),
        P("tp", "fs"),
        P("fs", "tp"),
        P("fs", "tp"),
        P("tp", "fs"),
    )
    return jax.shard_map(
        on_device,
        mesh=mesh,
        in_specs=placed,
        out_specs=(P(("rep", "fs"), None), P("tp", "fs"), P("tp")),
        check_vma=False,
    )
```

```python
import functools

import jax
import jax.numpy as jnp
from jax import lax
from jax.experimental import pallas as pl
from jax.experimental.pallas import tpu as pltpu
from jax.sharding import PartitionSpec as P

eps = 1e-06
f32, bf16 = jnp.float32, jnp.bfloat16


def kernel(sizes, tok, mid, cot, w1, w2, out, grad, norms, full1, full2, toks, mids, cots, mgs, xb, hidden, d_gate, d_up, mgt, part, got1, snd2, got2, dn, rs_out, rs_in, gb, nb, w_send, w_recv, own_sem, x_send, x_recv, s1_send, s1_recv, s2_send, s2_recv, s3_send, s3_recv, r_send, r_recv, g_send, g_recv, n_send, n_recv):
    R, F, T, n, D, H, pieces = sizes
    S, half, C, width = D // F, D // F // 2, D // T, 3 * H // pieces
    r, f, t = (lax.axis_index(a) for a in ("rep", "fs", "tp"))

    def fs_at(position):
        q = lax.rem(position + 2 * F, F)
        hi = q // (F // 2)
        return (1 - hi) * 2 * q + hi * (2 * (F - 1 - q) + 1)

    odd = lax.rem(f, 2)
    p = (1 - odd) * (f // 2) + odd * (F - 1 - f // 2)
    side = (fs_at(p + 1), fs_at(p - 1))

    barrier = pltpu.get_barrier_semaphore()
    for axis, size, me in (("rep", R, r), ("fs", F, f), ("tp", T, t)):
        for k in range(1, size):
            pl.semaphore_signal(barrier, inc=1, device_id={axis: lax.rem(me + k, size)}, device_id_type=pl.DeviceIdType.MESH)
    pl.semaphore_wait(barrier, R + F + T - 3)

    def remote(src, dst, send, recv, **where):
        return pltpu.make_async_remote_copy(src_ref=src, dst_ref=dst, send_sem=send, recv_sem=recv, device_id=where, device_id_type=pl.DeviceIdType.MESH)

    fulls = (full1, full2)

    def shard(b, d, distance, piece):
        owner = fs_at(p - distance if d == 0 else p + distance)
        rows = pl.ds(pl.multiple_of(owner * S + d * half, half), half)
        return fulls[b].at[rows, pl.ds(pl.multiple_of(piece * width, 128), width)]

    def ring(b, d, distance, step, piece):
        ref = shard(b, d, distance, piece)
        return remote(ref, ref, w_send.at[b, d], w_recv.at[b, d, step, piece], fs=side[d])

    def start_ring(b):
        for piece in range(pieces):
            for d in (0, 1):
                ring(b, d, 0, 0, piece).start()

    def serve(b, lo, hi):
        @pl.loop(lo, hi)
        def _(k):
            step, piece = k // pieces, lax.rem(k, pieces)
            for d in (0, 1):
                ring(b, d, step + 1, step, piece).wait_recv()
                ring(b, d, step + 1, step + 1, piece).start()

    relays = (F - 2) * pieces

    def upto(count):
        return relays * count // 18

    def end_ring(b):
        for piece in range(pieces):
            for d in (0, 1):
                ring(b, d, F - 1, F - 2, piece).wait_recv()

    def drain(b):
        whole = fulls[b].at[pl.ds(0, (F - 1) * half)]
        for d in (0, 1):
            remote(whole, whole, w_send.at[b, d], w_recv.at[b, d, 0, 0], fs=side[d]).wait_send()

    mine = pl.ds(pl.multiple_of(r * n, n), n)
    pairs = (mids, cots, toks, mgs)
    held = pl.ds(pl.multiple_of(f * S, S), S)
    loads = [pltpu.make_async_copy(src, dst, own_sem.at[i]) for i, (src, dst) in enumerate(((w2, full2.at[held]), (mid, mids.at[mine]), (cot, cots.at[mine]), (tok, toks.at[mine]), (w1, full1.at[held])))]
    for c in loads:
        c.start()

    def swap(i):
        return [remote(pairs[i].at[mine], pairs[i].at[mine], x_send.at[i, k - 1], x_recv.at[i, k - 1], rep=lax.rem(r + k, R)) for k in range(1, R)]

    def swap_in(i):
        for k in range(1, R):
            rows = pl.ds(pl.multiple_of(lax.rem(r + R - k, R) * n, n), n)
            remote(pairs[i].at[rows], pairs[i].at[rows], x_send.at[i, k - 1], x_recv.at[i, k - 1], rep=lax.rem(r + k, R)).wait_recv()

    loads[0].wait()
    start_ring(1)
    for i in range(3):
        loads[i + 1].wait()
        for c in swap(i):
            c.start()
    loads[4].wait()

    def normalise(pair):
        @pl.loop(0, R * n // 32)
        def _(i):
            rows = pl.ds(pl.multiple_of(i * 32, 32), 32)
            u = pair[rows, :].astype(f32)
            xb[rows, :] = (u * lax.rsqrt(jnp.mean(u * u, axis=1, keepdims=True) + eps)).astype(bf16)

    chunk = 256 if H % 256 == 0 else 128

    def forward(full, c_ref):
        @pl.loop(0, H // chunk)
        def _(j):
            def cols(which):
                return pl.ds(pl.multiple_of(which * H + j * chunk, 128), chunk)

            gate = jnp.dot(xb[...], full[:, cols(0)], preferred_element_type=f32)
            upper = jnp.dot(xb[...], full[:, cols(1)], preferred_element_type=f32)
            back = 0.5 * jnp.dot(c_ref[...], full[:, cols(2)], preferred_element_type=f32)
            logistic = jax.nn.sigmoid(gate)
            activated = gate * logistic
            hidden[:, cols(0)] = (activated * upper).astype(bf16)
            d_gate[:, cols(0)] = (back * upper * logistic * (1.0 + gate * (1.0 - logistic))).astype(bf16)
            d_up[:, cols(0)] = (back * activated).astype(bf16)

    dims = (((1,), (1,)), ((), ()))

    def backward(full, lo, hi):
        @pl.loop(lo, hi)
        def _(j):
            rows = pl.ds(pl.multiple_of(j * 256, 256), 256)
            total = lax.dot_general(d_gate[...], full[rows, 0:H], dims, preferred_element_type=f32)
            total = total + lax.dot_general(d_up[...], full[rows, H : 2 * H], dims, preferred_element_type=f32)
            part[:, rows] = total.astype(bf16)

    def block_of(k):
        return pl.ds(pl.multiple_of(k * C, 128), C)

    def stage1(b):
        return [remote(part.at[:, block_of(lax.rem(t + k, T))], got1.at[b, k - 1], s1_send.at[b, k - 1], s1_recv.at[b, k - 1], tp=lax.rem(t + k, T)) for k in range(1, T)]

    def stage2(b):
        return [remote(snd2.at[k - 1], got2.at[b, k - 1], s2_send.at[b, k - 1], s2_recv.at[b, k - 1], rep=lax.rem(r + k, R)) for k in range(1, R)]

    def stage3(b, owner):
        ref = dn.at[b, :, block_of(owner)]
        return lambda k: remote(ref, ref, s3_send.at[b, k - 1], s3_recv.at[b, k - 1], tp=lax.rem(t + k, T))

    def summed(b, base, i):
        rows = pl.ds(pl.multiple_of(base * n + i * 32, 32), 32)
        total = part[rows, block_of(t)].astype(f32)
        for k in range(T - 1):
            total = total + got1[b, k, rows, :].astype(f32)
        return total

    def reduce_tp(b):
        for c in stage1(b):
            c.wait()
        for k in range(1, R):
            @pl.loop(0, n // 32)
            def _(i, k=k):
                snd2[k - 1, pl.ds(pl.multiple_of(i * 32, 32), 32), :] = summed(b, lax.rem(r + k, R), i).astype(bf16)
        for c in stage2(b):
            c.start()

    def reduce_rep(b):
        for c in stage2(b):
            c.wait()

        @pl.loop(0, n // 32)
        def _(i):
            rows = pl.ds(pl.multiple_of(i * 32, 32), 32)
            total = summed(b, r, i)
            for k in range(R - 1):
                total = total + got2[b, k, rows, :].astype(f32)
            dn[b, rows, block_of(t)] = total.astype(bf16)

        for k in range(1, T):
            stage3(b, t)(k).start()

    def finish(b, pair, carried, result, offset):
        for k in range(1, T):
            stage3(b, lax.rem(t + T - k, T))(k).wait_recv()
            stage3(b, t)(k).wait_send()

        @pl.loop(0, n // 32)
        def _(i):
            rows = pl.ds(pl.multiple_of(i * 32, 32), 32)
            wide = pl.ds(pl.multiple_of(r * n + i * 32, 32), 32)
            u = pair[wide, :].astype(f32)
            scale = lax.rsqrt(jnp.mean(u * u, axis=1, keepdims=True) + eps)
            normed = u * scale
            d = dn[b, rows, :].astype(f32)
            d_u = carried[wide, :].astype(f32) + scale * (d - normed * jnp.mean(d * normed, axis=1, keepdims=True))
            result[pl.ds(pl.multiple_of(offset + i * 32, 32), 32), :] = d_u.astype(bf16)

    serve(1, 0, upto(10))
    swap_in(0)
    normalise(mids)
    serve(1, upto(10), upto(18))
    start_ring(0)
    swap_in(1)
    end_ring(1)
    forward(full2, cots)
    serve(0, 0, upto(1))
    backward(full2, 0, D // 512)
    serve(0, upto(1), upto(2))
    backward(full2, D // 512, D // 256)
    for c in stage1(1):
        c.start()
    serve(0, upto(2), upto(4))
    reduce_tp(1)
    swap_in(2)
    normalise(toks)
    serve(0, upto(4), upto(7))
    reduce_rep(1)
    serve(0, upto(7), upto(8))
    finish(1, mids, cots, mgs, r * n)
    for c in swap(3):
        c.start()
    serve(0, upto(8), upto(17))
    swap_in(3)

    @pl.loop(0, D // 256)
    def _(j):
        cols = pl.ds(pl.multiple_of(j * 256, 256), 256)
        mgt[cols, :] = mgs[:, cols].T

    serve(0, upto(17), upto(18))
    end_ring(0)

    forward(full1, mgs)

    def product(d, position):
        rows = pl.ds(pl.multiple_of(fs_at(position) * S + d * half, half), half)
        return 0.5 * jnp.dot(mgt[rows, :], hidden[...], preferred_element_type=f32)

    def rs(d, s):
        return remote(rs_out.at[d, s], rs_in.at[d, s], r_send.at[d, s], r_recv.at[d, s], fs=side[d])

    def passed(lo, hi):
        @pl.loop(lo, hi)
        def _(s):
            for d in (0, 1):
                value = product(d, p - 1 - s if d == 0 else p + 1 + s)
                rs(d, s - 1).wait_recv()
                rs_out[d, s] = (value + rs_in[d, s - 1].astype(f32)).astype(bf16)
                rs(d, s).start()

    def hop(count):
        return 1 + (F - 2) * count // 6

    for d in (0, 1):
        rs_out[d, 0] = product(d, p - 1 if d == 0 else p + 1).astype(bf16)
        rs(d, 0).start()
    backward(full1, 0, D // 256)
    for c in stage1(0):
        c.start()
    passed(1, hop(1))
    reduce_tp(0)
    passed(hop(1), hop(4))
    reduce_rep(0)
    passed(hop(4), hop(5))
    finish(0, toks, mgs, out, 0)
    passed(hop(5), hop(6))
    for d in (0, 1):
        value = product(d, p)
        rs(d, F - 2).wait_recv()
        gb[r, pl.ds(d * half, half), :] = (value + rs_in[d, F - 2].astype(f32)).astype(bf16)

    def trade(owner):
        return lambda k: remote(gb.at[owner], gb.at[owner], g_send.at[k - 1], g_recv.at[k - 1], rep=lax.rem(r + k, R))

    for k in range(1, R):
        trade(r)(k).start()
    for k in range(1, R):
        trade(lax.rem(r + R - k, R))(k).wait_recv()
        trade(r)(k).wait_send()
    for k in range(R):
        g = gb[k].astype(f32)
        grad[:, k * H : (k + 1) * H] = g
        nb[f, :, k * H : (k + 1) * H] = jnp.sum(g * g, axis=0, keepdims=True)

    def tell(owner):
        return lambda k: remote(nb.at[owner], nb.at[owner], n_send.at[k - 1], n_recv.at[k - 1], fs=lax.rem(f + k, F))

    for k in range(1, F):
        tell(f)(k).start()
    for b in (0, 1):
        drain(b)
    for i in range(4):
        for c in swap(i):
            c.wait_send()

    @pl.loop(0, F - 1)
    def _(s):
        for d in (0, 1):
            rs(d, s).wait_send()

    for k in range(1, F):
        tell(lax.rem(f + F - k, F))(k).wait_recv()
        tell(f)(k).wait_send()
    total = nb[0]
    for k in range(1, F):
        total = total + nb[k]
    norms[...] = total


def on_device(sizes, tokens, mid_tokens, out_grad, gate_first, up_first, down_first, gate_second, up_second, down_second):
    R, F, T, n, D, H, pieces = sizes
    S, half = D // F, D // F // 2
    start = lax.axis_index("rep") * H

    def own(gate_w, up_w, down_w):
        return jnp.concatenate(
            [
                lax.dynamic_slice_in_dim(gate_w, start, H, 1),
                lax.dynamic_slice_in_dim(up_w, start, H, 1),
                lax.dynamic_slice_in_dim(down_w, start, H, 0).T,
            ],
            axis=1,
        )

    dma = pltpu.SemaphoreType.DMA
    m = R * n
    any_space = pl.BlockSpec(memory_space=pl.ANY)
    vmem = pl.BlockSpec(memory_space=pltpu.VMEM)
    d_input, grad, norms = pl.pallas_call(
        functools.partial(kernel, sizes),
        out_shape=(
            jax.ShapeDtypeStruct((n, D), bf16),
            jax.ShapeDtypeStruct((S, R * H), f32),
            jax.ShapeDtypeStruct((1, R * H), f32),
        ),
        in_specs=[any_space] * 5,
        out_specs=(vmem, vmem, vmem),
        scratch_shapes=[
            pltpu.VMEM((D, 3 * H), bf16),
            pltpu.VMEM((D, 3 * H), bf16),
            pltpu.VMEM((m, D), bf16),
            pltpu.VMEM((m, D), bf16),
            pltpu.VMEM((m, D), bf16),
            pltpu.VMEM((m, D), bf16),
            pltpu.VMEM((m, D), bf16),
            pltpu.VMEM((m, H), bf16),
            pltpu.VMEM((m, H), bf16),
            pltpu.VMEM((m, H), bf16),
            pltpu.VMEM((D, m), bf16),
            pltpu.VMEM((m, D), bf16),
            pltpu.VMEM((2, T - 1, m, D // T), bf16),
            pltpu.VMEM((R - 1, n, D // T), bf16),
            pltpu.VMEM((2, R - 1, n, D // T), bf16),
            pltpu.VMEM((2, n, D), bf16),
            pltpu.VMEM((2, F - 1, half, H), bf16),
            pltpu.VMEM((2, F - 1, half, H), bf16),
            pltpu.VMEM((R, S, H), bf16),
            pltpu.VMEM((F, 1, R * H), f32),
            dma((2, 2)),
            dma((2, 2, F - 1, pieces)),
            dma((5,)),
            dma((4, R - 1)),
            dma((4, R - 1)),
            dma((2, T - 1)),
            dma((2, T - 1)),
            dma((2, R - 1)),
            dma((2, R - 1)),
            dma((2, T - 1)),
            dma((2, T - 1)),
            dma((2, F - 1)),
            dma((2, F - 1)),
            dma((R - 1,)),
            dma((R - 1,)),
            dma((F - 1,)),
            dma((F - 1,)),
        ],
        compiler_params=pltpu.CompilerParams(
            collective_id=0, has_side_effects=True, vmem_limit_bytes=67043328
        ),
    )(
        tokens,
        mid_tokens,
        out_grad,
        own(gate_first, up_first, down_first),
        own(gate_second, up_second, down_second),
    )
    return d_input, grad.T, norms.reshape(-1)


def solution(mesh):
    R, F, T = (mesh.shape[a] for a in ("rep", "fs", "tp"))

    def whole(tokens, mid_tokens, out_grad, gate_first, *rest):
        D, FF = gate_first.shape
        sizes = (R, F, T, tokens.shape[0] // (R * F), D, FF // (T * R), 3 if F <= 8 else 1)
        return jax.shard_map(
            functools.partial(on_device, sizes),
            mesh=mesh,
            in_specs=(P(("rep", "fs"), None),) * 3 + (P("fs", "tp"), P("fs", "tp"), P("tp", "fs")) * 2,
            out_specs=(P(("rep", "fs"), None), P("tp", "fs"), P("tp")),
            check_vma=False,
        )(tokens, mid_tokens, out_grad, gate_first, *rest)

    return whole
```

```python
import functools

import jax
import jax.numpy as jnp
from jax import lax
from jax.experimental import pallas as pl
from jax.experimental.pallas import tpu as pltpu
from jax.sharding import PartitionSpec as P

eps = 1e-06
f32, bf16 = jnp.float32, jnp.bfloat16


def kernel(sizes, tok, mid, cot, w1, v1, w2, v2, out, grad, norms, full1, downs1, full2, downs2, toks, mids, cots, mgs, xb, hidden, d_gate, d_up, mgt, gates, uppers, part, got1, snd2, got2, dn, rs_out, rs_in, gb, nb, w_send, w_recv, own_sem, x_send, x_recv, s1_send, s1_recv, s2_send, s2_recv, s3_send, s3_recv, r_send, r_recv, g_send, g_recv, n_send, n_recv):
    R, F, T, n, D, H, pieces = sizes
    S, half, C, width = D // F, D // F // 2, D // T, H // pieces
    both = 2 if pieces > 1 else 1
    r, f, t = (lax.axis_index(a) for a in ("rep", "fs", "tp"))

    def fs_at(position):
        q = lax.rem(position + 2 * F, F)
        hi = q // (F // 2)
        return (1 - hi) * 2 * q + hi * (2 * (F - 1 - q) + 1)

    odd = lax.rem(f, 2)
    p = (1 - odd) * (f // 2) + odd * (F - 1 - f // 2)
    side = (fs_at(p + 1), fs_at(p - 1))

    barrier = pltpu.get_barrier_semaphore()
    for axis, size, me in (("rep", R, r), ("fs", F, f), ("tp", T, t)):
        for k in range(1, size):
            pl.semaphore_signal(barrier, inc=1, device_id={axis: lax.rem(me + k, size)}, device_id_type=pl.DeviceIdType.MESH)
    pl.semaphore_wait(barrier, R + F + T - 3)

    def remote(src, dst, send, recv, **where):
        return pltpu.make_async_remote_copy(src_ref=src, dst_ref=dst, send_sem=send, recv_sem=recv, device_id=where, device_id_type=pl.DeviceIdType.MESH)

    fulls = ((full1, downs1), (full2, downs2))

    second_gu, second_d = (1, 0, both, 2 * H // both, 0), (1, 1, pieces, width, both)
    first_gu, first_d = (0,) + second_gu[1:], (0,) + second_d[1:]

    def ring(phase, d, distance, step, piece):
        b, which, count, wide, sem = phase
        owner = fs_at(p - distance if d == 0 else p + distance)
        rows = pl.ds(pl.multiple_of(owner * S + d * half, half), half)
        ref = fulls[b][which].at[rows]
        if count > 1:
            ref = fulls[b][which].at[rows, pl.ds(pl.multiple_of(piece * wide, 128), wide)]
        return remote(ref, ref, w_send.at[b, which, d], w_recv.at[b, d, step, sem + piece], fs=side[d])

    def start_ring(phase):
        for piece in range(phase[2]):
            for d in (0, 1):
                ring(phase, d, 0, 0, piece).start()

    def serve(phase, lo, hi, of):
        relays = (F - 2) * phase[2]

        @pl.loop(relays * lo // of, relays * hi // of)
        def _(k):
            step, piece = k // phase[2], lax.rem(k, phase[2])
            for d in (0, 1):
                ring(phase, d, step + 1, step, piece).wait_recv()
                ring(phase, d, step + 1, step + 1, piece).start()

    def end_ring(phase):
        for piece in range(phase[2]):
            for d in (0, 1):
                ring(phase, d, F - 1, F - 2, piece).wait_recv()

    def drain(b):
        for which in (0, 1):
            whole = fulls[b][which].at[pl.ds(0, (F - 1) * half)]
            for d in (0, 1):
                remote(whole, whole, w_send.at[b, which, d], w_recv.at[b, d, 0, 0], fs=side[d]).wait_send()

    mine = pl.ds(pl.multiple_of(r * n, n), n)
    pairs = (mids, cots, toks, mgs)
    held = pl.ds(pl.multiple_of(f * S, S), S)
    loads = [pltpu.make_async_copy(src, dst, own_sem.at[i]) for i, (src, dst) in enumerate(((w2, full2.at[held]), (mid, mids.at[mine]), (cot, cots.at[mine]), (tok, toks.at[mine]), (v2, downs2.at[held]), (w1, full1.at[held]), (v1, downs1.at[held])))]
    for c in loads:
        c.start()

    def swap(i):
        return [remote(pairs[i].at[mine], pairs[i].at[mine], x_send.at[i, k - 1], x_recv.at[i, k - 1], rep=lax.rem(r + k, R)) for k in range(1, R)]

    def swap_in(i):
        for k in range(1, R):
            rows = pl.ds(pl.multiple_of(lax.rem(r + R - k, R) * n, n), n)
            remote(pairs[i].at[rows], pairs[i].at[rows], x_send.at[i, k - 1], x_recv.at[i, k - 1], rep=lax.rem(r + k, R)).wait_recv()

    loads[0].wait()
    start_ring(second_gu)
    for i in range(3):
        loads[i + 1].wait()
        for c in swap(i):
            c.start()
    for c in loads[4:]:
        c.wait()

    def normalise(pair):
        @pl.loop(0, R * n // 32)
        def _(i):
            rows = pl.ds(pl.multiple_of(i * 32, 32), 32)
            u = pair[rows, :].astype(f32)
            xb[rows, :] = (u * lax.rsqrt(jnp.mean(u * u, axis=1, keepdims=True) + eps)).astype(bf16)

    chunk = 256 if H % 256 == 0 else 128 if H % 128 == 0 else H

    def cols(which, j):
        if chunk == H:
            return pl.ds(which * H, H)
        return pl.ds(pl.multiple_of(which * H + j * chunk, 128), chunk)

    def forward(full):
        @pl.loop(0, H // chunk)
        def _(j):
            gate = jnp.dot(xb[...], full[:, cols(0, j)], preferred_element_type=f32)
            upper = jnp.dot(xb[...], full[:, cols(1, j)], preferred_element_type=f32)
            hidden[:, cols(0, j)] = (gate * jax.nn.sigmoid(gate) * upper).astype(bf16)
            gates[:, cols(0, j)] = gate
            uppers[:, cols(0, j)] = upper

    def backed(downs, c_ref):
        @pl.loop(0, H // chunk)
        def _(j):
            gate, upper = gates[:, cols(0, j)], uppers[:, cols(0, j)]
            back = 0.5 * jnp.dot(c_ref[...], downs[:, cols(0, j)], preferred_element_type=f32)
            logistic = jax.nn.sigmoid(gate)
            d_gate[:, cols(0, j)] = (back * upper * logistic * (1.0 + gate * (1.0 - logistic))).astype(bf16)
            d_up[:, cols(0, j)] = (back * gate * logistic).astype(bf16)

    dims = (((1,), (1,)), ((), ()))

    def backward(full, lo, hi):
        @pl.loop(lo, hi)
        def _(j):
            rows = pl.ds(pl.multiple_of(j * 256, 256), 256)
            total = lax.dot_general(d_gate[...], full[rows, 0:H], dims, preferred_element_type=f32)
            total = total + lax.dot_general(d_up[...], full[rows, H : 2 * H], dims, preferred_element_type=f32)
            part[:, rows] = total.astype(bf16)

    def block_of(k):
        return pl.ds(pl.multiple_of(k * C, 128), C)

    def stage1(b):
        return [remote(part.at[:, block_of(lax.rem(t + k, T))], got1.at[b, k - 1], s1_send.at[b, k - 1], s1_recv.at[b, k - 1], tp=lax.rem(t + k, T)) for k in range(1, T)]

    def stage2(b):
        return [remote(snd2.at[k - 1], got2.at[b, k - 1], s2_send.at[b, k - 1], s2_recv.at[b, k - 1], rep=lax.rem(r + k, R)) for k in range(1, R)]

    def stage3(b, owner):
        ref = dn.at[b, :, block_of(owner)]
        return lambda k: remote(ref, ref, s3_send.at[b, k - 1], s3_recv.at[b, k - 1], tp=lax.rem(t + k, T))

    def summed(b, base, i):
        rows = pl.ds(pl.multiple_of(base * n + i * 32, 32), 32)
        total = part[rows, block_of(t)].astype(f32)
        for k in range(T - 1):
            total = total + got1[b, k, rows, :].astype(f32)
        return total

    def reduce_tp(b):
        for c in stage1(b):
            c.wait()
        for k in range(1, R):
            @pl.loop(0, n // 32)
            def _(i, k=k):
                snd2[k - 1, pl.ds(pl.multiple_of(i * 32, 32), 32), :] = summed(b, lax.rem(r + k, R), i).astype(bf16)
        for c in stage2(b):
            c.start()

    def reduce_rep(b):
        for c in stage2(b):
            c.wait()

        @pl.loop(0, n // 32)
        def _(i):
            rows = pl.ds(pl.multiple_of(i * 32, 32), 32)
            total = summed(b, r, i)
            for k in range(R - 1):
                total = total + got2[b, k, rows, :].astype(f32)
            dn[b, rows, block_of(t)] = total.astype(bf16)

        for k in range(1, T):
            stage3(b, t)(k).start()

    def finish(b, pair, carried, result, offset):
        for k in range(1, T):
            stage3(b, lax.rem(t + T - k, T))(k).wait_recv()
            stage3(b, t)(k).wait_send()

        @pl.loop(0, n // 32)
        def _(i):
            rows = pl.ds(pl.multiple_of(i * 32, 32), 32)
            wide = pl.ds(pl.multiple_of(r * n + i * 32, 32), 32)
            u = pair[wide, :].astype(f32)
            scale = lax.rsqrt(jnp.mean(u * u, axis=1, keepdims=True) + eps)
            normed = u * scale
            d = dn[b, rows, :].astype(f32)
            d_u = carried[wide, :].astype(f32) + scale * (d - normed * jnp.mean(d * normed, axis=1, keepdims=True))
            result[pl.ds(pl.multiple_of(offset + i * 32, 32), 32), :] = d_u.astype(bf16)

    serve(second_gu, 0, 10, 12)
    swap_in(0)
    normalise(mids)
    serve(second_gu, 10, 12, 12)
    start_ring(second_d)
    end_ring(second_gu)
    serve(second_d, 0, 3, 18)
    forward(full2)
    serve(second_d, 3, 18, 18)
    start_ring(first_gu)
    swap_in(1)
    end_ring(second_d)
    backed(downs2, cots)
    serve(first_gu, 0, 1, 12)
    backward(full2, 0, D // 512)
    serve(first_gu, 1, 2, 12)
    backward(full2, D // 512, D // 256)
    for c in stage1(1):
        c.start()
    serve(first_gu, 2, 3, 12)
    reduce_tp(1)
    serve(first_gu, 3, 4, 12)
    swap_in(2)
    normalise(toks)
    serve(first_gu, 4, 6, 12)
    reduce_rep(1)
    serve(first_gu, 6, 7, 12)
    finish(1, mids, cots, mgs, r * n)
    for c in swap(3):
        c.start()
    serve(first_gu, 7, 12, 12)
    start_ring(first_d)
    end_ring(first_gu)

    forward(full1)
    serve(first_d, 0, 6, 18)
    swap_in(3)

    @pl.loop(0, D // 256)
    def _(j):
        part_cols = pl.ds(pl.multiple_of(j * 256, 256), 256)
        mgt[part_cols, :] = mgs[:, part_cols].T

    serve(first_d, 6, 18, 18)

    def strip(piece):
        return pl.ds(pl.multiple_of(piece * width, 128), width) if pieces > 1 else slice(None)

    def product(d, position, piece):
        rows = pl.ds(pl.multiple_of(fs_at(position) * S + d * half, half), half)
        return 0.5 * jnp.dot(mgt[rows, :], hidden[:, strip(piece)], preferred_element_type=f32)

    def view(ref, piece):
        return ref.at[:, strip(piece)] if pieces > 1 else ref

    def rs(d, s, piece):
        return remote(view(rs_out.at[d, s], piece), view(rs_in.at[d, s], piece), r_send.at[d, s, piece], r_recv.at[d, s, piece], fs=side[d])

    def passed(lo, hi):
        @pl.loop(1 + (F - 2) * lo // 6, 1 + (F - 2) * hi // 6)
        def _(s):
            for piece in range(pieces):
                for d in (0, 1):
                    value = product(d, p - 1 - s if d == 0 else p + 1 + s, piece)
                    rs(d, s - 1, piece).wait_recv()
                    rs_out[d, s, :, strip(piece)] = (value + rs_in[d, s - 1, :, strip(piece)].astype(f32)).astype(bf16)
                    rs(d, s, piece).start()

    for piece in range(pieces):
        for d in (0, 1):
            rs_out[d, 0, :, strip(piece)] = product(d, p - 1 if d == 0 else p + 1, piece).astype(bf16)
            rs(d, 0, piece).start()
    end_ring(first_d)
    backed(downs1, mgs)
    passed(0, 1)
    backward(full1, 0, D // 512)
    passed(1, 2)
    backward(full1, D // 512, D // 256)
    for c in stage1(0):
        c.start()
    passed(2, 3)
    reduce_tp(0)
    passed(3, 6)

    def trade(owner, piece):
        ref = view(gb.at[owner], piece)
        return lambda k: remote(ref, ref, g_send.at[k - 1, piece], g_recv.at[k - 1, piece], rep=lax.rem(r + k, R))

    for piece in range(pieces):
        for d in (0, 1):
            value = product(d, p, piece)
            rs(d, F - 2, piece).wait_recv()
            gb[r, pl.ds(d * half, half), strip(piece)] = (value + rs_in[d, F - 2, :, strip(piece)].astype(f32)).astype(bf16)
        for k in range(1, R):
            trade(r, piece)(k).start()
    reduce_rep(0)
    finish(0, toks, mgs, out, 0)
    for piece in range(pieces):
        for k in range(1, R):
            trade(lax.rem(r + R - k, R), piece)(k).wait_recv()
            trade(r, piece)(k).wait_send()
    for k in range(R):
        g = gb[k].astype(f32)
        grad[:, k * H : (k + 1) * H] = g
        nb[f, :, k * H : (k + 1) * H] = jnp.sum(g * g, axis=0, keepdims=True)

    def tell(owner):
        return lambda k: remote(nb.at[owner], nb.at[owner], n_send.at[k - 1], n_recv.at[k - 1], fs=lax.rem(f + k, F))

    for k in range(1, F):
        tell(f)(k).start()
    for b in (0, 1):
        drain(b)
    for i in range(4):
        for c in swap(i):
            c.wait_send()

    @pl.loop(0, F - 1)
    def _(s):
        for piece in range(pieces):
            for d in (0, 1):
                rs(d, s, piece).wait_send()

    for k in range(1, F):
        tell(lax.rem(f + F - k, F))(k).wait_recv()
        tell(f)(k).wait_send()
    total = nb[0]
    for k in range(1, F):
        total = total + nb[k]
    norms[...] = total


def on_device(sizes, tokens, mid_tokens, out_grad, gate_first, up_first, down_first, gate_second, up_second, down_second):
    R, F, T, n, D, H, pieces = sizes
    S, half = D // F, D // F // 2
    start = lax.axis_index("rep") * H

    def own(gate_w, up_w, down_w):
        pair = [lax.dynamic_slice_in_dim(w, start, H, 1) for w in (gate_w, up_w)]
        return jnp.concatenate(pair, axis=1), lax.dynamic_slice_in_dim(down_w, start, H, 0).T

    dma = pltpu.SemaphoreType.DMA
    m = R * n
    any_space = pl.BlockSpec(memory_space=pl.ANY)
    vmem = pl.BlockSpec(memory_space=pltpu.VMEM)
    d_input, grad, norms = pl.pallas_call(
        functools.partial(kernel, sizes),
        out_shape=(
            jax.ShapeDtypeStruct((n, D), bf16),
            jax.ShapeDtypeStruct((S, R * H), f32),
            jax.ShapeDtypeStruct((1, R * H), f32),
        ),
        in_specs=[any_space] * 7,
        out_specs=(vmem, vmem, vmem),
        scratch_shapes=[
            pltpu.VMEM((D, 2 * H), bf16),
            pltpu.VMEM((D, H), bf16),
            pltpu.VMEM((D, 2 * H), bf16),
            pltpu.VMEM((D, H), bf16),
            pltpu.VMEM((m, D), bf16),
            pltpu.VMEM((m, D), bf16),
            pltpu.VMEM((m, D), bf16),
            pltpu.VMEM((m, D), bf16),
            pltpu.VMEM((m, D), bf16),
            pltpu.VMEM((m, H), bf16),
            pltpu.VMEM((m, H), bf16),
            pltpu.VMEM((m, H), bf16),
            pltpu.VMEM((D, m), bf16),
            pltpu.VMEM((m, H), f32),
            pltpu.VMEM((m, H), f32),
            pltpu.VMEM((m, D), bf16),
            pltpu.VMEM((2, T - 1, m, D // T), bf16),
            pltpu.VMEM((R - 1, n, D // T), bf16),
            pltpu.VMEM((2, R - 1, n, D // T), bf16),
            pltpu.VMEM((2, n, D), bf16),
            pltpu.VMEM((2, F - 1, half, H), bf16),
            pltpu.VMEM((2, F - 1, half, H), bf16),
            pltpu.VMEM((R, S, H), bf16),
            pltpu.VMEM((F, 1, R * H), f32),
            dma((2, 2, 2)),
            dma((2, 2, F - 1, pieces + (2 if pieces > 1 else 1))),
            dma((7,)),
            dma((4, R - 1)),
            dma((4, R - 1)),
            dma((2, T - 1)),
            dma((2, T - 1)),
            dma((2, R - 1)),
            dma((2, R - 1)),
            dma((2, T - 1)),
            dma((2, T - 1)),
            dma((2, F - 1, pieces)),
            dma((2, F - 1, pieces)),
            dma((R - 1, pieces)),
            dma((R - 1, pieces)),
            dma((F - 1,)),
            dma((F - 1,)),
        ],
        compiler_params=pltpu.CompilerParams(
            collective_id=0, has_side_effects=True, vmem_limit_bytes=67043328
        ),
    )(
        tokens,
        mid_tokens,
        out_grad,
        *own(gate_first, up_first, down_first),
        *own(gate_second, up_second, down_second),
    )
    return d_input, grad.T, norms.reshape(-1)


def solution(mesh):
    R, F, T = (mesh.shape[a] for a in ("rep", "fs", "tp"))

    def whole(tokens, mid_tokens, out_grad, gate_first, *rest):
        D, FF = gate_first.shape
        sizes = (R, F, T, tokens.shape[0] // (R * F), D, FF // (T * R), 3 if F <= 8 and FF // (T * R) % 384 == 0 else 1)
        return jax.shard_map(
            functools.partial(on_device, sizes),
            mesh=mesh,
            in_specs=(P(("rep", "fs"), None),) * 3 + (P("fs", "tp"), P("fs", "tp"), P("tp", "fs")) * 2,
            out_specs=(P(("rep", "fs"), None), P("tp", "fs"), P("tp")),
            check_vma=False,
        )(tokens, mid_tokens, out_grad, gate_first, *rest)

    return whole
```

```python
import functools

import jax
import jax.numpy as jnp
from jax import lax
from jax.experimental import pallas as pl
from jax.experimental.pallas import tpu as pltpu
from jax.sharding import PartitionSpec as P

eps = 1e-06
f32, bf16 = jnp.float32, jnp.bfloat16


def kernel(sizes, tok, mid, cot, g1, u1, v1, g2, u2, v2, out, grad, norms, full1, downs1, full2, downs2, toks, mids, cots, mgs, xb, hidden, d_gate, d_up, mgt, gates, uppers, part, got1, snd2, got2, dn, rs_out, rs_in, gb, nb, w_send, w_recv, own_sem, x_send, x_recv, s1_send, s1_recv, s2_send, s2_recv, s3_send, s3_recv, r_send, r_recv, g_send, g_recv, n_send, n_recv):
    R, F, T, n, D, H, pieces = sizes
    S, half, C, width = D // F, D // F // 2, D // T, H // pieces
    both = 2 if pieces > 1 else 1
    r, f, t = (lax.axis_index(a) for a in ("rep", "fs", "tp"))

    def fs_at(position):
        q = lax.rem(position + 2 * F, F)
        hi = q // (F // 2)
        return (1 - hi) * 2 * q + hi * (2 * (F - 1 - q) + 1)

    odd = lax.rem(f, 2)
    p = (1 - odd) * (f // 2) + odd * (F - 1 - f // 2)
    side = (fs_at(p + 1), fs_at(p - 1))

    barrier = pltpu.get_barrier_semaphore()
    for axis, size, me in (("rep", R, r), ("fs", F, f), ("tp", T, t)):
        for k in range(1, size):
            pl.semaphore_signal(barrier, inc=1, device_id={axis: lax.rem(me + k, size)}, device_id_type=pl.DeviceIdType.MESH)
    pl.semaphore_wait(barrier, R + F + T - 3)

    def remote(src, dst, send, recv, **where):
        return pltpu.make_async_remote_copy(src_ref=src, dst_ref=dst, send_sem=send, recv_sem=recv, device_id=where, device_id_type=pl.DeviceIdType.MESH)

    fulls = ((full1, downs1), (full2, downs2))

    second_gu, second_d = (1, 0, both, 2 * H // both, 0), (1, 1, pieces, width, both)
    first_gu, first_d = (0,) + second_gu[1:], (0,) + second_d[1:]

    def ring(phase, d, distance, step, piece):
        b, which, count, wide, sem = phase
        owner = fs_at(p - distance if d == 0 else p + distance)
        rows = pl.ds(pl.multiple_of(owner * S + d * half, half), half)
        ref = fulls[b][which].at[rows]
        if count > 1:
            ref = fulls[b][which].at[rows, pl.ds(pl.multiple_of(piece * wide, 128), wide)]
        return remote(ref, ref, w_send.at[b, which, d], w_recv.at[b, d, step, sem + piece], fs=side[d])

    def start_ring(phase):
        for piece in range(phase[2]):
            for d in (0, 1):
                ring(phase, d, 0, 0, piece).start()

    def serve(phase, lo, hi, of):
        relays = (F - 2) * phase[2]

        @pl.loop(relays * lo // of, relays * hi // of)
        def _(k):
            step, piece = k // phase[2], lax.rem(k, phase[2])
            for d in (0, 1):
                ring(phase, d, step + 1, step, piece).wait_recv()
                ring(phase, d, step + 1, step + 1, piece).start()

    def end_ring(phase):
        for piece in range(phase[2]):
            for d in (0, 1):
                ring(phase, d, F - 1, F - 2, piece).wait_recv()

    def drain(b):
        for which in (0, 1):
            whole = fulls[b][which].at[pl.ds(0, (F - 1) * half)]
            for d in (0, 1):
                remote(whole, whole, w_send.at[b, which, d], w_recv.at[b, d, 0, 0], fs=side[d]).wait_send()

    mine = pl.ds(pl.multiple_of(r * n, n), n)
    pairs = (mids, cots, toks, mgs)
    held = pl.ds(pl.multiple_of(f * S, S), S)
    def pair_loads(g, u, full):
        if H % 128 > 0:
            return [(g, full.at[held])]
        taken = pl.ds(pl.multiple_of(r * H, 128), H)
        return [(g.at[:, taken], full.at[held, pl.ds(0, H)]), (u.at[:, taken], full.at[held, pl.ds(H, H)])]

    wanted = pair_loads(g2, u2, full2)
    ahead = len(wanted)
    wanted += [(mid, mids.at[mine]), (cot, cots.at[mine]), (tok, toks.at[mine]), (v2, downs2.at[held]), (v1, downs1.at[held])]
    wanted += pair_loads(g1, u1, full1)
    loads = [pltpu.make_async_copy(src, dst, own_sem.at[i]) for i, (src, dst) in enumerate(wanted)]
    for c in loads:
        c.start()

    def swap(i):
        return [remote(pairs[i].at[mine], pairs[i].at[mine], x_send.at[i, k - 1], x_recv.at[i, k - 1], rep=lax.rem(r + k, R)) for k in range(1, R)]

    def swap_in(i):
        for k in range(1, R):
            rows = pl.ds(pl.multiple_of(lax.rem(r + R - k, R) * n, n), n)
            remote(pairs[i].at[rows], pairs[i].at[rows], x_send.at[i, k - 1], x_recv.at[i, k - 1], rep=lax.rem(r + k, R)).wait_recv()

    for c in loads[:ahead]:
        c.wait()
    start_ring(second_gu)
    for i in range(3):
        loads[ahead + i].wait()
        for c in swap(i):
            c.start()
    for c in loads[ahead + 3 :]:
        c.wait()

    def normalise(pair):
        @pl.loop(0, R * n // 32)
        def _(i):
            rows = pl.ds(pl.multiple_of(i * 32, 32), 32)
            u = pair[rows, :].astype(f32)
            xb[rows, :] = (u * lax.rsqrt(jnp.mean(u * u, axis=1, keepdims=True) + eps)).astype(bf16)

    chunk = 256 if H % 256 == 0 else 128 if H % 128 == 0 else H

    def cols(which, j):
        if chunk == H:
            return pl.ds(which * H, H)
        return pl.ds(pl.multiple_of(which * H + j * chunk, 128), chunk)

    def forward(full):
        @pl.loop(0, H // chunk)
        def _(j):
            gate = jnp.dot(xb[...], full[:, cols(0, j)], preferred_element_type=f32)
            upper = jnp.dot(xb[...], full[:, cols(1, j)], preferred_element_type=f32)
            hidden[:, cols(0, j)] = (gate * jax.nn.sigmoid(gate) * upper).astype(bf16)
            gates[:, cols(0, j)] = gate
            uppers[:, cols(0, j)] = upper

    def backed(downs, c_ref):
        @pl.loop(0, H // chunk)
        def _(j):
            gate, upper = gates[:, cols(0, j)], uppers[:, cols(0, j)]
            back = 0.5 * jnp.dot(c_ref[...], downs[:, cols(0, j)], preferred_element_type=f32)
            logistic = jax.nn.sigmoid(gate)
            d_gate[:, cols(0, j)] = (back * upper * logistic * (1.0 + gate * (1.0 - logistic))).astype(bf16)
            d_up[:, cols(0, j)] = (back * gate * logistic).astype(bf16)

    dims = (((1,), (1,)), ((), ()))

    def backward(full, lo, hi):
        @pl.loop(lo, hi)
        def _(j):
            rows = pl.ds(pl.multiple_of(j * 256, 256), 256)
            total = lax.dot_general(d_gate[...], full[rows, 0:H], dims, preferred_element_type=f32)
            total = total + lax.dot_general(d_up[...], full[rows, H : 2 * H], dims, preferred_element_type=f32)
            part[:, rows] = total.astype(bf16)

    def block_of(k):
        return pl.ds(pl.multiple_of(k * C, 128), C)

    def stage1(b):
        return [remote(part.at[:, block_of(lax.rem(t + k, T))], got1.at[b, k - 1], s1_send.at[b, k - 1], s1_recv.at[b, k - 1], tp=lax.rem(t + k, T)) for k in range(1, T)]

    def stage2(b):
        return [remote(snd2.at[k - 1], got2.at[b, k - 1], s2_send.at[b, k - 1], s2_recv.at[b, k - 1], rep=lax.rem(r + k, R)) for k in range(1, R)]

    def stage3(b, owner):
        ref = dn.at[b, :, block_of(owner)]
        return lambda k: remote(ref, ref, s3_send.at[b, k - 1], s3_recv.at[b, k - 1], tp=lax.rem(t + k, T))

    def summed(b, base, i):
        rows = pl.ds(pl.multiple_of(base * n + i * 32, 32), 32)
        total = part[rows, block_of(t)].astype(f32)
        for k in range(T - 1):
            total = total + got1[b, k, rows, :].astype(f32)
        return total

    def reduce_tp(b):
        for c in stage1(b):
            c.wait()
        for k in range(1, R):
            @pl.loop(0, n // 32)
            def _(i, k=k):
                snd2[k - 1, pl.ds(pl.multiple_of(i * 32, 32), 32), :] = summed(b, lax.rem(r + k, R), i).astype(bf16)
        for c in stage2(b):
            c.start()

    def reduce_rep(b):
        for c in stage2(b):
            c.wait()

        @pl.loop(0, n // 32)
        def _(i):
            rows = pl.ds(pl.multiple_of(i * 32, 32), 32)
            total = summed(b, r, i)
            for k in range(R - 1):
                total = total + got2[b, k, rows, :].astype(f32)
            dn[b, rows, block_of(t)] = total.astype(bf16)

        for k in range(1, T):
            stage3(b, t)(k).start()

    def finish(b, pair, carried, result, offset):
        for k in range(1, T):
            stage3(b, lax.rem(t + T - k, T))(k).wait_recv()
            stage3(b, t)(k).wait_send()

        @pl.loop(0, n // 32)
        def _(i):
            rows = pl.ds(pl.multiple_of(i * 32, 32), 32)
            wide = pl.ds(pl.multiple_of(r * n + i * 32, 32), 32)
            u = pair[wide, :].astype(f32)
            scale = lax.rsqrt(jnp.mean(u * u, axis=1, keepdims=True) + eps)
            normed = u * scale
            d = dn[b, rows, :].astype(f32)
            d_u = carried[wide, :].astype(f32) + scale * (d - normed * jnp.mean(d * normed, axis=1, keepdims=True))
            result[pl.ds(pl.multiple_of(offset + i * 32, 32), 32), :] = d_u.astype(bf16)

    serve(second_gu, 0, 10, 12)
    swap_in(0)
    normalise(mids)
    serve(second_gu, 10, 12, 12)
    start_ring(second_d)
    end_ring(second_gu)
    serve(second_d, 0, 3, 18)
    forward(full2)
    serve(second_d, 3, 18, 18)
    start_ring(first_gu)
    swap_in(1)
    end_ring(second_d)
    backed(downs2, cots)
    serve(first_gu, 0, 1, 12)
    backward(full2, 0, D // 512)
    serve(first_gu, 1, 2, 12)
    backward(full2, D // 512, D // 256)
    for c in stage1(1):
        c.start()
    serve(first_gu, 2, 3, 12)
    reduce_tp(1)
    serve(first_gu, 3, 4, 12)
    swap_in(2)
    normalise(toks)
    serve(first_gu, 4, 6, 12)
    reduce_rep(1)
    serve(first_gu, 6, 7, 12)
    finish(1, mids, cots, mgs, r * n)
    for c in swap(3):
        c.start()
    serve(first_gu, 7, 12, 12)
    start_ring(first_d)
    end_ring(first_gu)

    forward(full1)
    serve(first_d, 0, 6, 18)
    swap_in(3)

    @pl.loop(0, D // 256)
    def _(j):
        part_cols = pl.ds(pl.multiple_of(j * 256, 256), 256)
        mgt[part_cols, :] = mgs[:, part_cols].T

    serve(first_d, 6, 18, 18)

    def strip(piece):
        return pl.ds(pl.multiple_of(piece * width, 128), width) if pieces > 1 else slice(None)

    def product(d, position, piece):
        rows = pl.ds(pl.multiple_of(fs_at(position) * S + d * half, half), half)
        return 0.5 * jnp.dot(mgt[rows, :], hidden[:, strip(piece)], preferred_element_type=f32)

    def view(ref, piece):
        return ref.at[:, strip(piece)] if pieces > 1 else ref

    def rs(d, s, piece):
        return remote(view(rs_out.at[d, s], piece), view(rs_in.at[d, s], piece), r_send.at[d, s, piece], r_recv.at[d, s, piece], fs=side[d])

    def passed(lo, hi):
        @pl.loop(1 + (F - 2) * lo // 6, 1 + (F - 2) * hi // 6)
        def _(s):
            for piece in range(pieces):
                for d in (0, 1):
                    value = product(d, p - 1 - s if d == 0 else p + 1 + s, piece)
                    rs(d, s - 1, piece).wait_recv()
                    rs_out[d, s, :, strip(piece)] = (value + rs_in[d, s - 1, :, strip(piece)].astype(f32)).astype(bf16)
                    rs(d, s, piece).start()

    for piece in range(pieces):
        for d in (0, 1):
            rs_out[d, 0, :, strip(piece)] = product(d, p - 1 if d == 0 else p + 1, piece).astype(bf16)
            rs(d, 0, piece).start()
    end_ring(first_d)
    backed(downs1, mgs)
    passed(0, 1)
    backward(full1, 0, D // 512)
    passed(1, 2)
    backward(full1, D // 512, D // 256)
    for c in stage1(0):
        c.start()
    passed(2, 3)
    reduce_tp(0)
    passed(3, 6)

    def trade(owner, piece):
        ref = view(gb.at[owner], piece)
        return lambda k: remote(ref, ref, g_send.at[k - 1, piece], g_recv.at[k - 1, piece], rep=lax.rem(r + k, R))

    for piece in range(pieces):
        for d in (0, 1):
            value = product(d, p, piece)
            rs(d, F - 2, piece).wait_recv()
            gb[r, pl.ds(d * half, half), strip(piece)] = (value + rs_in[d, F - 2, :, strip(piece)].astype(f32)).astype(bf16)
        for k in range(1, R):
            trade(r, piece)(k).start()
    reduce_rep(0)
    finish(0, toks, mgs, out, 0)
    for piece in range(pieces):
        for k in range(1, R):
            trade(lax.rem(r + R - k, R), piece)(k).wait_recv()
            trade(r, piece)(k).wait_send()
    for k in range(R):
        g = gb[k].astype(f32)
        grad[:, k * H : (k + 1) * H] = g
        nb[f, :, k * H : (k + 1) * H] = jnp.sum(g * g, axis=0, keepdims=True)

    def tell(owner):
        return lambda k: remote(nb.at[owner], nb.at[owner], n_send.at[k - 1], n_recv.at[k - 1], fs=lax.rem(f + k, F))

    for k in range(1, F):
        tell(f)(k).start()
    for b in (0, 1):
        drain(b)
    for i in range(4):
        for c in swap(i):
            c.wait_send()

    @pl.loop(0, F - 1)
    def _(s):
        for piece in range(pieces):
            for d in (0, 1):
                rs(d, s, piece).wait_send()

    for k in range(1, F):
        tell(lax.rem(f + F - k, F))(k).wait_recv()
        tell(f)(k).wait_send()
    total = nb[0]
    for k in range(1, F):
        total = total + nb[k]
    norms[...] = total


def on_device(sizes, tokens, mid_tokens, out_grad, gate_first, up_first, down_first, gate_second, up_second, down_second):
    R, F, T, n, D, H, pieces = sizes
    S, half = D // F, D // F // 2
    start = lax.axis_index("rep") * H

    def own(gate_w, up_w, down_w):
        down = lax.dynamic_slice_in_dim(down_w, start, H, 0).T
        if H % 128 == 0:
            return gate_w, up_w, down
        pair = [lax.dynamic_slice_in_dim(w, start, H, 1) for w in (gate_w, up_w)]
        return jnp.concatenate(pair, axis=1), up_w, down

    dma = pltpu.SemaphoreType.DMA
    m = R * n
    any_space = pl.BlockSpec(memory_space=pl.ANY)
    vmem = pl.BlockSpec(memory_space=pltpu.VMEM)
    d_input, grad, norms = pl.pallas_call(
        functools.partial(kernel, sizes),
        out_shape=(
            jax.ShapeDtypeStruct((n, D), bf16),
            jax.ShapeDtypeStruct((S, R * H), f32),
            jax.ShapeDtypeStruct((1, R * H), f32),
        ),
        in_specs=[any_space] * 9,
        out_specs=(vmem, vmem, vmem),
        scratch_shapes=[
            pltpu.VMEM((D, 2 * H), bf16),
            pltpu.VMEM((D, H), bf16),
            pltpu.VMEM((D, 2 * H), bf16),
            pltpu.VMEM((D, H), bf16),
            pltpu.VMEM((m, D), bf16),
            pltpu.VMEM((m, D), bf16),
            pltpu.VMEM((m, D), bf16),
            pltpu.VMEM((m, D), bf16),
            pltpu.VMEM((m, D), bf16),
            pltpu.VMEM((m, H), bf16),
            pltpu.VMEM((m, H), bf16),
            pltpu.VMEM((m, H), bf16),
            pltpu.VMEM((D, m), bf16),
            pltpu.VMEM((m, H), f32),
            pltpu.VMEM((m, H), f32),
            pltpu.VMEM((m, D), bf16),
            pltpu.VMEM((2, T - 1, m, D // T), bf16),
            pltpu.VMEM((R - 1, n, D // T), bf16),
            pltpu.VMEM((2, R - 1, n, D // T), bf16),
            pltpu.VMEM((2, n, D), bf16),
            pltpu.VMEM((2, F - 1, half, H), bf16),
            pltpu.VMEM((2, F - 1, half, H), bf16),
            pltpu.VMEM((R, S, H), bf16),
            pltpu.VMEM((F, 1, R * H), f32),
            dma((2, 2, 2)),
            dma((2, 2, F - 1, pieces + (2 if pieces > 1 else 1))),
            dma((9,)),
            dma((4, R - 1)),
            dma((4, R - 1)),
            dma((2, T - 1)),
            dma((2, T - 1)),
            dma((2, R - 1)),
            dma((2, R - 1)),
            dma((2, T - 1)),
            dma((2, T - 1)),
            dma((2, F - 1, pieces)),
            dma((2, F - 1, pieces)),
            dma((R - 1, pieces)),
            dma((R - 1, pieces)),
            dma((F - 1,)),
            dma((F - 1,)),
        ],
        compiler_params=pltpu.CompilerParams(
            collective_id=0, has_side_effects=True, vmem_limit_bytes=67043328
        ),
    )(
        tokens,
        mid_tokens,
        out_grad,
        *own(gate_first, up_first, down_first),
        *own(gate_second, up_second, down_second),
    )
    return d_input, grad.T, norms.reshape(-1)


def solution(mesh):
    R, F, T = (mesh.shape[a] for a in ("rep", "fs", "tp"))

    def whole(tokens, mid_tokens, out_grad, gate_first, *rest):
        D, FF = gate_first.shape
        sizes = (R, F, T, tokens.shape[0] // (R * F), D, FF // (T * R), 3 if F <= 8 and FF // (T * R) % 384 == 0 else 1)
        return jax.shard_map(
            functools.partial(on_device, sizes),
            mesh=mesh,
            in_specs=(P(("rep", "fs"), None),) * 3 + (P("fs", "tp"), P("fs", "tp"), P("tp", "fs")) * 2,
            out_specs=(P(("rep", "fs"), None), P("tp", "fs"), P("tp")),
            check_vma=False,
        )(tokens, mid_tokens, out_grad, gate_first, *rest)

    return whole
```
